32 devices in a mesh: sp: 8 (over z, y), tp: 4 (over x, core).
Axes of the slice: x: 2, y: 2, z: 4, core: 2. Of those that a mesh axis runs over, the one named last changes fastest.
Arguments:
- queries: bfloat16 [4096, 1024], P('sp', 'tp'), may hold values from -60 to 60
- keys: bfloat16 [4096, 1024], P('sp', 'tp'), may hold values from -6 to 6
- values: bfloat16 [4096, 1024], P('sp', 'tp'), may hold values from -6 to 6
- lambdas: float32 [8], P('tp'), may hold values from 0.3 to 0.8
- head_gain: float32 [128], replicated, may hold values from 0.1 to 1.9
- w_out: bfloat16 [1024, 2048], replicated, may hold values from -0.1875 to 0.1875
- residual_in: bfloat16 [4096, 2048], P(('sp', 'tp')), may hold values from -6 to 6
- norm_gain: float32 [2048], replicated, may hold values from 0.1 to 1.9
- route_ids: int32 [4096, 2], P(('sp', 'tp')), may hold values from 0 to 7, as said below
- route_weight: float32 [4096, 2], P(('sp', 'tp')), may hold values from 0.2 to 1
- w_gate: bfloat16 [8, 2048, 1024], P('sp', None, 'tp'), may hold values from -0.125 to 0.125
- w_up: bfloat16 [8, 2048, 1024], P('sp', None, 'tp'), may hold values from -0.125 to 0.125
- w_down: bfloat16 [8, 2048, 1024], P('sp', None, 'tp'), may hold values from -0.1875 to 0.1875
Outputs:
- layer_out: bfloat16 [4096, 2048], P(('sp', 'tp'))
The draws below stay inside these ranges and needn't reach their ends.
Inputs may be any that keep to these rules, and one draw needn't show every extreme that they name: `route_ids`: each row names two different experts of one group (the same expert // 8). Among the 128 rows of one device (aligned blocks), no expert is named more than 64 times, and in every draw one expert is named exactly 64 times in the rows of every device.
All inputs are finite; a program needn't handle non-finite values.
Results may differ from the reference program's by a relative error of at most 0.015.
Values may be sent and summed in bfloat16 or wider, within the bound.
No kernel may reach another device: no remote copies, remote signals or barrier semaphores. Data moves between devices by JAX's collectives and lax.ppermute only.
A program may use at most 128 MiB of HBM per device.

```python
import jax
import jax.numpy as jnp
from jax import lax

D = 2048
HEADS = 8
HEAD_DIM = 64
FF = 1024
GROUP_SIZE = 8
SEQ_LEN = 4096
SEQUENCES = 1
TOKENS = 4096
DEV_ROWS = 128
EXPERTS = 8
GROUPS = 1
CAPACITY = 64


def base_field(key, salt_value):
    array_shape = (TOKENS, HEADS * 2 * HEAD_DIM)
    subkey = jax.random.fold_in(key, salt_value)
    return jnp.clip(1.3 * jax.random.normal(subkey, array_shape, jnp.float32), -5.5, 5.5)


def draw_keys(key, part):
    base_values = base_field(key, 11)
    return base_values.astype(jnp.bfloat16)


def draw_queries(key, part):
    base_values = base_field(key, 12)
    return base_values.astype(jnp.bfloat16)


def draw_route_ids(key, part):
    block_count = TOKENS // DEV_ROWS
    pair_count = EXPERTS * CAPACITY // 2
    favored = jax.random.randint(jax.random.fold_in(key, 31), (), 0, EXPERTS)
    round_offsets = (jnp.arange(GROUPS * CAPACITY, dtype=jnp.int32) // CAPACITY)[:, None] * GROUP_SIZE

    def one_block(block_key):
        round_keys = jax.random.split(jax.random.fold_in(block_key, 1), GROUPS * CAPACITY)
        rounds = jax.vmap(lambda round_key: jax.random.permutation(round_key, GROUP_SIZE))(round_keys)
        pair_table = (rounds.astype(jnp.int32) + round_offsets).reshape(pair_count, 2)
        holds_favored = jnp.any(pair_table == favored, axis=1).astype(jnp.int32)
        jitter_values = jax.random.randint(jax.random.fold_in(block_key, 2), (pair_count,), 0, 1 << 18)
        priority = (jitter_values + holds_favored * (1 << 18)) * pair_count + jnp.arange(pair_count, dtype=jnp.int32)
        unused, picked = lax.top_k(priority, DEV_ROWS)
        shuffle = jax.random.permutation(jax.random.fold_in(block_key, 3), DEV_ROWS)
        return pair_table[picked][shuffle]
    block_keys = jax.vmap(lambda block_index: jax.random.fold_in(jax.random.fold_in(key, 32), block_index))(jnp.arange(block_count))
    return jax.vmap(one_block)(block_keys).reshape(TOKENS, 2).astype(jnp.int32)


def steps_of(own_key, shape, shards, low, largest):
    level = 1.0
    for position, parts in shards:
        steps = jax.random.uniform(jax.random.fold_in(jax.random.fold_in(own_key, 6), position), (parts,), jnp.float32, low / len(shards), largest / len(shards))
        level = level * jnp.repeat(jnp.exp(steps), shape[position] // parts).reshape((-1,) + (1,) * (len(shape) - 1 - position))
    return level


def scatter_about(stream_key, shape, deviation, reach, shards=(), held_as=jnp.bfloat16):
    drawn = deviation * jax.random.normal(stream_key, shape, jnp.float32)
    if shards:
        drawn = drawn * steps_of(stream_key, shape, shards, -0.22, 0.18)
    return jnp.clip(drawn, -reach, reach).astype(held_as)


def setup_inputs(seed: int = 0) -> dict:
    splits = jax.random.split(jax.random.key(seed), 14)
    queries = draw_queries(jax.random.fold_in(splits[13], 71), 0)
    keys = draw_keys(jax.random.fold_in(splits[13], 71), 0)
    values = scatter_about(splits[2], (TOKENS, HEADS * 2 * HEAD_DIM), 1.0, 6.0, ((0, 8), (1, 4)))
    lambdas = jnp.clip(0.3 + 0.5 * jax.random.uniform(splits[3], (HEADS,), jnp.float32) ** steps_of(splits[3], (HEADS,), ((0, 4),), -0.2, 0.2), 0.3, 0.8)
    head_gain = jnp.clip(1.0 + 0.18 * jax.random.normal(splits[4], (2 * HEAD_DIM,), jnp.float32), 0.1, 1.9)
    w_out = scatter_about(splits[5], (HEADS * 2 * HEAD_DIM, D), (HEADS * 2 * HEAD_DIM) ** -0.5, 0.1875)
    residual_in = scatter_about(splits[6], (TOKENS, D), 1.0, 6.0, ((0, 32),))
    norm_gain = jnp.clip(1.0 + 0.18 * jax.random.normal(splits[7], (D,), jnp.float32), 0.1, 1.9)
    route_ids = draw_route_ids(jax.random.fold_in(splits[13], 71), 0)
    route_weight = jnp.clip(0.2 + 0.8 * jax.random.uniform(splits[9], (TOKENS, 2), jnp.float32) ** steps_of(splits[9], (TOKENS, 2), ((0, 32),), -0.2, 0.2), 0.2, 1.0)
    w_gate = scatter_about(splits[10], (EXPERTS, D, FF), D ** -0.5, 0.125, ((0, 8), (2, 4)))
    w_up = scatter_about(splits[11], (EXPERTS, D, FF), D ** -0.5, 0.125, ((0, 8), (2, 4)))
    w_down = scatter_about(splits[12], (EXPERTS, D, FF), FF ** -0.5, 0.1875, ((0, 8), (2, 4)))
    return {"queries": queries, "keys": keys, "values": values, "lambdas": lambdas, "head_gain": head_gain, "w_out": w_out, "residual_in": residual_in, "norm_gain": norm_gain, "route_ids": route_ids, "route_weight": route_weight, "w_gate": w_gate, "w_up": w_up, "w_down": w_down}


EPSILON = 1e-06
OUT_SCALE = 0.8

def slot_numbers(flat_ids):
    count_ids = flat_ids.shape[0]
    positions = lax.broadcasted_iota(jnp.int32, (count_ids, count_ids), 0)
    earlier = lax.broadcasted_iota(jnp.int32, (count_ids, count_ids), 1) < positions
    matches = (flat_ids[:, None] == flat_ids[None, :]) & earlier
    return lax.optimization_barrier(jnp.sum(matches.astype(jnp.int32), axis=1))

def attend_block(query_block, key_view, value_view, lambdas, head_gain):
    scores = jnp.einsum('qhmd,khmd->hmqk', query_block.astype(jnp.float32), key_view) * HEAD_DIM ** (-0.5)
    peak_score = lax.optimization_barrier(jnp.max(scores, axis=-1, keepdims=True))
    weights = jnp.exp(scores - peak_score)
    totals = lax.optimization_barrier(jnp.sum(weights, axis=-1))
    rounded = lax.optimization_barrier(weights.astype(jnp.bfloat16)).astype(jnp.float32)
    numerators = jnp.einsum('hmqk,khv->hmqv', rounded, value_view)
    heads_out = numerators / totals[..., None]
    combined = heads_out[:, 0] - lambdas[:, None, None] * heads_out[:, 1]
    mean_square = lax.optimization_barrier(jnp.mean(combined * combined, axis=-1, keepdims=True))
    normalized = combined * lax.rsqrt(mean_square + EPSILON) * head_gain * OUT_SCALE
    return jnp.transpose(normalized, (1, 0, 2)).reshape(query_block.shape[0], -1).astype(jnp.bfloat16)

def attend_sequence(operands, lambdas, head_gain):
    seq_queries, seq_keys, seq_values = operands
    query_view = seq_queries.reshape(SEQ_LEN // 128, 128, HEADS, 2, HEAD_DIM)
    key_view = seq_keys.reshape(SEQ_LEN, HEADS, 2, HEAD_DIM).astype(jnp.float32)
    value_view = seq_values.reshape(SEQ_LEN, HEADS, 2 * HEAD_DIM).astype(jnp.float32)
    return lax.map(lambda query_block: attend_block(query_block, key_view, value_view, lambdas, head_gain), query_view)

def run_expert(operands):
    rows_in, gate_weight, up_weight, down_weight = operands
    gate_proj = jnp.dot(rows_in, gate_weight, preferred_element_type=jnp.float32)
    up_proj = jnp.dot(rows_in, up_weight, preferred_element_type=jnp.float32)
    hidden_units = (jax.nn.silu(gate_proj) * up_proj).astype(jnp.bfloat16)
    return jnp.dot(hidden_units, down_weight.T, preferred_element_type=jnp.float32).astype(jnp.bfloat16)

def reference(queries, keys, values, lambdas, head_gain, w_out, residual_in, norm_gain, route_ids, route_weight, w_gate, w_up, w_down):
    width = HEADS * 2 * HEAD_DIM
    seq_shape = (SEQUENCES, SEQ_LEN, width)
    attended = lax.map(lambda operands: attend_sequence(operands, lambdas, head_gain), (queries.reshape(seq_shape), keys.reshape(seq_shape), values.reshape(seq_shape)))
    attended = attended.reshape(TOKENS, width)
    mixed_out = jnp.dot(attended, w_out, preferred_element_type=jnp.float32).astype(jnp.bfloat16)
    carried = (residual_in.astype(jnp.float32) + mixed_out.astype(jnp.float32)).astype(jnp.bfloat16)
    carried_wide = carried.astype(jnp.float32)
    normed = (carried_wide * lax.rsqrt(lax.optimization_barrier(jnp.mean(carried_wide * carried_wide, axis=-1, keepdims=True)) + EPSILON) * norm_gain).astype(jnp.bfloat16)
    blocks = TOKENS // DEV_ROWS
    flat_ids = route_ids.reshape(blocks, 2 * DEV_ROWS)
    slot_index = jax.vmap(slot_numbers)(flat_ids)
    targets = (flat_ids * CAPACITY + slot_index).astype(jnp.int32)
    sources = jnp.repeat(normed.reshape(blocks, DEV_ROWS, D), 2, axis=1)
    block_index = jnp.broadcast_to(jnp.arange(blocks, dtype=jnp.int32)[:, None], targets.shape)
    buffers = jnp.zeros((blocks, EXPERTS * CAPACITY, D), jnp.bfloat16).at[block_index, targets].set(sources)
    per_expert = jnp.moveaxis(buffers.reshape(blocks, EXPERTS, CAPACITY, D), 1, 0).reshape(EXPERTS, blocks * CAPACITY, D)
    outputs = lax.map(run_expert, (per_expert, w_gate, w_up, w_down))
    returned = jnp.moveaxis(outputs.reshape(EXPERTS, blocks, CAPACITY, D), 0, 1).reshape(blocks, EXPERTS * CAPACITY, D)
    picked = returned[block_index, targets].astype(jnp.float32).reshape(TOKENS, 2, D)
    layer_out = carried.astype(jnp.float32) + lax.optimization_barrier(jnp.sum(route_weight[..., None] * picked, axis=1))
    return layer_out.astype(jnp.bfloat16)
```

```python
import functools

import jax
import jax.numpy as jnp
from jax import lax
from jax.experimental import pallas as pl
from jax.experimental.pallas import tpu as pltpu
from jax.sharding import PartitionSpec as P

EPSILON = 1e-06
OUT_SCALE = 0.8
FLOOR_SCORE = -1e30
LOG2_E = 1.4426950408889634


def moved(value, destination):
    layers = lax.axis_size("sp") // 2
    pairs = []
    for z in range(layers):
        for y in range(2):
            for x in range(2):
                for c in range(2):
                    dz, dy, dx, dc = destination(z, y, x, c)
                    pairs.append(((2 * z + y) * 4 + 2 * x + c, (2 * dz + dy) * 4 + 2 * dx + dc))
    return lax.ppermute(value, ("sp", "tp"), pairs)


def attention_kernel(lam_ref, query_ref, *refs, key_pieces, head_dim, score_scale):
    piece_refs = refs[:key_pieces]
    gain_ref, out_ref = refs[key_pieces], refs[key_pieces + 1]
    query = query_ref[...]
    rows = query.shape[0]
    value_dim = 2 * head_dim
    first_map = lax.broadcasted_iota(jnp.int32, query.shape, 1) < head_dim
    zeros = jnp.zeros_like(query)
    both = jnp.concatenate(
        [jnp.where(first_map, query, zeros), jnp.where(first_map, zeros, query)], axis=0
    )
    factor = score_scale * LOG2_E
    scores = []
    peak = None
    for piece in piece_refs:
        part = lax.dot_general(
            both, piece[0], (((1,), (1,)), ((), ())), preferred_element_type=jnp.float32
        )
        scores.append(part)
        part_peak = jnp.max(part, axis=1, keepdims=True)
        peak = part_peak if peak is None else jnp.maximum(peak, part_peak)
    total = jnp.zeros((2 * rows, 2 * value_dim), jnp.float32)
    for part, piece in zip(scores, piece_refs):
        weights = jnp.exp2((part - peak) * factor).astype(jnp.bfloat16)
        value = piece[1]
        extended = jnp.concatenate([value, jnp.ones_like(value)], axis=1)
        total = total + jnp.dot(weights, extended, preferred_element_type=jnp.float32)
    heads_out = total[:, :value_dim] / total[:, value_dim:]
    combined = heads_out[:rows] - lam_ref[0] * heads_out[rows:]
    mean_square = jnp.mean(combined * combined, axis=1, keepdims=True)
    normalized = combined * lax.rsqrt(mean_square + EPSILON) * gain_ref[...] * OUT_SCALE
    out_ref[...] = normalized.astype(jnp.bfloat16)


def attention(lam, query, pieces, gain, head_dim, block_rows=128):
    rows, width = query.shape
    block_rows = min(block_rows, rows)
    whole = [pl.BlockSpec(piece.shape, lambda i: (0, 0, 0)) for piece in pieces]
    return pl.pallas_call(
        functools.partial(
            attention_kernel,
            key_pieces=len(pieces),
            head_dim=head_dim,
            score_scale=head_dim ** (-0.5),
        ),
        grid=(rows // block_rows,),
        in_specs=[
            pl.BlockSpec(memory_space=pltpu.SMEM),
            pl.BlockSpec((block_rows, width), lambda i: (i, 0)),
            *whole,
            pl.BlockSpec((1, width), lambda i: (0, 0)),
        ],
        out_specs=pl.BlockSpec((block_rows, width), lambda i: (i, 0)),
        out_shape=jax.ShapeDtypeStruct((rows, width), jnp.bfloat16),
        name="attention",
    )(lam.reshape(1), query, *pieces, gain.reshape(1, width))


def spread_attention(queries, keys, values, lambdas, head_gain):
    layers = lax.axis_size("sp") // 2
    tok_rows = queries.shape[0]
    width = queries.shape[1] // 2
    own_rows = tok_rows // 4
    z = lax.axis_index("sp") // 2
    x = lax.axis_index("tp") // 2
    c = lax.axis_index("tp") % 2

    stacked = jnp.stack([queries, keys, values]).reshape(3, 2, 2, own_rows, 2, width)
    messages = jnp.transpose(stacked, (4, 2, 0, 1, 3, 5)).reshape(4, 3, 2 * own_rows, width)
    pieces = []
    for k in range(layers):
        message = lax.dynamic_index_in_dim(messages, z ^ k, 0, keepdims=False)
        pieces.append(
            moved(message, lambda z, y, x, c: (2 * c + ((z ^ k) >> 1), y, x, (z ^ k) & 1))
        )
    other_lambdas = moved(lambdas, lambda z, y, x, c: (z, y, x, 1 - c))
    both_lambdas = jnp.where(z // 2 == c, lambdas, other_lambdas)
    lam = lax.dynamic_index_in_dim(both_lambdas, z % 2, 0, keepdims=False)

    first = jnp.stack([pieces[0][1:], pieces[1][1:]], axis=1).reshape(2, 4 * own_rows, width)
    second = jnp.stack([pieces[2][1:], pieces[3][1:]], axis=1).reshape(2, 4 * own_rows, width)
    y_swap = lambda z, y, x, c: (z, 1 - y, x, c)
    c_swap = lambda z, y, x, c: (z, y, x, 1 - c)
    chip = [first, second, moved(first, y_swap), moved(second, y_swap)]
    held = chip + [moved(piece, c_swap) for piece in chip]

    query_rows = jnp.stack([piece[0] for piece in pieces]).reshape(layers, 2, own_rows, width)
    other_query = lax.dynamic_index_in_dim(query_rows, 1 - x, 1, keepdims=False)
    own_query = lax.dynamic_index_in_dim(query_rows, x, 1, keepdims=False)
    head_dim = width // 2
    other_att = attention(lam, other_query.reshape(-1, width), held, head_gain, head_dim)
    came_att = moved(other_att, lambda z, y, x, c: (z, y, 1 - x, c))
    own_att = attention(lam, own_query.reshape(-1, width), held, head_gain, head_dim)
    pair = jnp.stack(
        [own_att.reshape(layers, own_rows, width), came_att.reshape(layers, own_rows, width)],
        axis=1,
    )
    source = (z % 2) * 2 + c
    gathered = []
    for step in range(layers):
        part = lax.dynamic_index_in_dim(pair, source ^ z ^ step, 0, keepdims=False)
        if step:
            part = moved(part, lambda z, y, x, c: (z ^ step, y, x, c))
        gathered.append(part)
    everything = jnp.stack(gathered)
    ordered = []
    for head_x in range(2):
        for head_z in range(layers):
            row = lax.dynamic_index_in_dim(everything, z ^ head_z, 0, keepdims=False)
            ordered.append(lax.dynamic_index_in_dim(row, x ^ head_x, 0, keepdims=False))
    return jnp.concatenate(ordered, axis=1), own_att


def slot_numbers(flat_ids):
    count_ids = flat_ids.shape[0]
    positions = lax.broadcasted_iota(jnp.int32, (count_ids, count_ids), 0)
    earlier = lax.broadcasted_iota(jnp.int32, (count_ids, count_ids), 1) < positions
    matches = (flat_ids[:, None] == flat_ids[None, :]) & earlier
    return jnp.sum(matches.astype(jnp.int32), axis=1)


def normalize(carried_wide, norm_gain):
    return (
        carried_wide
        * lax.rsqrt(jnp.mean(carried_wide * carried_wide, axis=-1, keepdims=True) + EPSILON)
        * norm_gain
    ).astype(jnp.bfloat16)


def ffn_kernel(rows_ref, *refs, shards):
    gate_refs, up_refs, down_refs = refs[:shards], refs[shards : 2 * shards], refs[2 * shards : 3 * shards]
    out_ref = refs[3 * shards]
    gate_vmem, up_vmem, down_vmem, sems = refs[3 * shards + 1 :]
    copies = []
    for s in range(shards):
        copies.append(pltpu.make_async_copy(gate_refs[s], gate_vmem.at[s], sems.at[0, s]))
        copies.append(pltpu.make_async_copy(up_refs[s], up_vmem.at[s], sems.at[1, s]))
        copies.append(pltpu.make_async_copy(down_refs[s], down_vmem.at[s], sems.at[2, s]))
    for copy in copies:
        copy.start()
    rows = rows_ref[...]
    total = None
    for s in range(shards):
        copies[3 * s].wait()
        gate = jnp.dot(rows, gate_vmem[s], preferred_element_type=jnp.float32)
        copies[3 * s + 1].wait()
        up = jnp.dot(rows, up_vmem[s], preferred_element_type=jnp.float32)
        hidden = (gate / (1.0 + jnp.exp(-gate)) * up).astype(jnp.bfloat16)
        copies[3 * s + 2].wait()
        part = lax.dot_general(
            hidden, down_vmem[s], (((1,), (1,)), ((), ())), preferred_element_type=jnp.float32
        )
        total = part if total is None else total + part
    out_ref[...] = total.astype(jnp.bfloat16)


def expert_ffn(rows, gates, ups, downs):
    shards = len(gates)
    count, width = rows.shape
    shape = gates[0].shape
    anywhere = pl.BlockSpec(memory_space=pl.ANY)
    return pl.pallas_call(
        functools.partial(ffn_kernel, shards=shards),
        in_specs=[pl.BlockSpec(memory_space=pltpu.VMEM)] + [anywhere] * (3 * shards),
        out_specs=pl.BlockSpec(memory_space=pltpu.VMEM),
        out_shape=jax.ShapeDtypeStruct((count, width), jnp.bfloat16),
        scratch_shapes=[
            pltpu.VMEM((shards,) + shape, jnp.bfloat16),
            pltpu.VMEM((shards,) + shape, jnp.bfloat16),
            pltpu.VMEM((shards,) + shape, jnp.bfloat16),
            pltpu.SemaphoreType.DMA((3, shards)),
        ],
        name="expert_ffn",
    )(rows, *gates, *ups, *downs)


def spread_layer(
    queries, keys, values, lambdas, head_gain, w_out, residual_in, norm_gain,
    route_ids, route_weight, w_gate, w_up, w_down,
):
    x_swap = lambda z, y, x, c: (z, y, 1 - x, c)
    c_swap = lambda z, y, x, c: (z, y, x, 1 - c)

    def shards_of(weight):
        own = weight[0]
        far = moved(own, x_swap)
        return [own, moved(own, c_swap), far, moved(far, c_swap)]

    attended, own_att = spread_attention(queries, keys, values, lambdas, head_gain)
    gates = shards_of(w_gate)
    ups = shards_of(w_up)
    late_down, unused = lax.optimization_barrier((w_down, own_att))
    downs = shards_of(late_down)

    mixed_out = jnp.dot(attended, w_out, preferred_element_type=jnp.float32).astype(jnp.bfloat16)
    carried = (residual_in.astype(jnp.float32) + mixed_out.astype(jnp.float32)).astype(jnp.bfloat16)
    carried_wide = carried.astype(jnp.float32)
    normed = normalize(carried_wide, norm_gain)
    dev_rows, model_width = normed.shape
    devices = lax.axis_size("sp")
    expert_count = w_gate.shape[0] * devices
    capacity = max(2, 4 * dev_rows // expert_count)
    chunks = 2 if capacity % 32 == 0 else 1
    piece = capacity // chunks
    flat_ids = route_ids.reshape(-1)
    slots = slot_numbers(flat_ids)
    targets = (
        (slots // piece) * (expert_count * piece) + flat_ids * piece + slots % piece
    ).reshape(dev_rows, 2)
    total_slots = expert_count * capacity
    slot_rows = lax.broadcasted_iota(jnp.int32, (total_slots, dev_rows), 0)
    placement = (
        (slot_rows == targets[:, 0][None, :]) | (slot_rows == targets[:, 1][None, :])
    ).astype(jnp.bfloat16)
    slot_columns = lax.broadcasted_iota(jnp.int32, (dev_rows, total_slots), 1)
    picks = [(slot_columns == targets[:, k][:, None]).astype(jnp.bfloat16) for k in range(2)]
    chunk_rows = expert_count * piece
    returned = []
    for chunk in range(chunks):
        span = slice(chunk * chunk_rows, (chunk + 1) * chunk_rows)
        outgoing = jnp.dot(
            placement[span], normed, preferred_element_type=jnp.float32
        ).astype(jnp.bfloat16)
        arrived = lax.all_to_all(
            outgoing.reshape(devices, piece, model_width), "sp", 0, 0, tiled=True
        )
        results = expert_ffn(arrived.reshape(chunk_rows, model_width), gates, ups, downs)
        came = lax.all_to_all(
            results.reshape(devices, piece, model_width), "sp", 0, 0, tiled=True
        )
        returned.append(came.reshape(chunk_rows, model_width))
    summed = None
    for k in range(2):
        picked = None
        for chunk in range(chunks):
            span = slice(chunk * chunk_rows, (chunk + 1) * chunk_rows)
            part = jnp.dot(picks[k][:, span], returned[chunk], preferred_element_type=jnp.float32)
            picked = part if picked is None else picked + part
        weighted = route_weight[:, k][:, None] * picked
        summed = weighted if summed is None else summed + weighted
    return (carried_wide + summed).astype(jnp.bfloat16)


def swapped(value, axis, distance):
    mask = 2**distance
    pairs = [(source, source ^ mask) for source in range(lax.axis_size(axis))]
    return lax.ppermute(value, axis, pairs)


def block_length(total_rows):
    largest = 1
    for divisor in range(1, min(total_rows, 1024) + 1):
        if total_rows % divisor == 0:
            largest = divisor
    return largest


def expert_hidden(arrived, gate_weight, up_weight):
    gate_proj = jnp.einsum(
        "secd,edf->secf", arrived, gate_weight, preferred_element_type=jnp.float32
    )
    up_proj = jnp.einsum("secd,edf->secf", arrived, up_weight, preferred_element_type=jnp.float32)
    return (jax.nn.silu(gate_proj) * up_proj).astype(jnp.bfloat16)


def send_back(results):
    return lax.all_to_all(results, "sp", split_axis=0, concat_axis=0, tiled=True)


def local(
    queries,
    keys,
    values,
    lambdas,
    head_gain,
    w_out,
    residual_in,
    norm_gain,
    route_ids,
    route_weight,
    w_gate,
    w_up,
    w_down,
):
    tok_rows = queries.shape[0]
    local_heads = lambdas.shape[0]
    head_dim = queries.shape[1] // (2 * local_heads)
    value_dim = 2 * head_dim
    score_scale = head_dim ** (-0.5)
    query_view = queries.reshape(tok_rows, local_heads, 2, head_dim)

    def absorb(running, key_piece, value_piece):
        key_count = key_piece.shape[0]
        step_rows = block_length(key_count)
        key_blocks = key_piece.reshape(key_count // step_rows, step_rows, local_heads, 2, head_dim)
        value_blocks = value_piece.reshape(
            key_count // step_rows, step_rows, local_heads, value_dim
        )

        def one_block(state, block_pair):
            key_block, value_block = block_pair
            running_max, running_sum, running_acc = state
            scores = (
                jnp.einsum(
                    "qhmd,khmd->hmqk", query_view, key_block, preferred_element_type=jnp.float32
                )
                * score_scale
            )
            new_max = jnp.maximum(running_max, jnp.max(scores, axis=-1))
            weights = jnp.exp(scores - new_max[..., None])
            shrink = jnp.exp(running_max - new_max)
            new_sum = running_sum * shrink + jnp.sum(weights, axis=-1)
            product = jnp.einsum(
                "hmqk,khv->hmqv",
                weights.astype(jnp.bfloat16),
                value_block,
                preferred_element_type=jnp.float32,
            )
            return ((new_max, new_sum, running_acc * shrink[..., None] + product), None)

        final_state, unused = lax.scan(one_block, running, (key_blocks, value_blocks))
        return final_state

    initial = (
        jnp.full((local_heads, 2, tok_rows), FLOOR_SCORE, jnp.float32),
        jnp.zeros((local_heads, 2, tok_rows), jnp.float32),
        jnp.zeros((local_heads, 2, tok_rows, value_dim), jnp.float32),
    )
    seq_bits = min(4, lax.axis_size("sp").bit_length() - 1)
    held_keys, held_values = (keys, values)
    state = absorb(initial, held_keys, held_values)
    for bit_number in range(seq_bits):
        came_keys, came_values = swapped((held_keys, held_values), "sp", bit_number)
        state = absorb(state, came_keys, came_values)
        if bit_number + 1 < seq_bits:
            held_keys = jnp.concatenate([held_keys, came_keys], axis=0)
            held_values = jnp.concatenate([held_values, came_values], axis=0)
    peaks, totals, numerators = state
    heads_out = numerators / totals[..., None]
    combined = heads_out[:, 0] - lambdas[:, None, None] * heads_out[:, 1]
    mean_square = jnp.mean(combined * combined, axis=-1, keepdims=True)
    normalized = combined * lax.rsqrt(mean_square + EPSILON) * head_gain * OUT_SCALE
    attended = (
        jnp.transpose(normalized, (1, 0, 2))
        .reshape(tok_rows, local_heads * value_dim)
        .astype(jnp.bfloat16)
    )
    dev_rows = residual_in.shape[0]
    head_width = attended.shape[1]
    own_rows = lax.dynamic_slice_in_dim(w_out, lax.axis_index("tp") * head_width, head_width, 0)
    mixed_sum = lax.psum_scatter(
        jnp.dot(attended, own_rows, preferred_element_type=jnp.float32).astype(jnp.bfloat16),
        "tp",
        scatter_dimension=0,
        tiled=True,
    )
    carried = (residual_in.astype(jnp.float32) + mixed_sum.astype(jnp.float32)).astype(jnp.bfloat16)
    carried_wide = carried.astype(jnp.float32)
    normed = (
        carried_wide
        * lax.rsqrt(jnp.mean(carried_wide * carried_wide, axis=-1, keepdims=True) + EPSILON)
        * norm_gain
    ).astype(jnp.bfloat16)
    model_width = normed.shape[1]
    experts_here = w_gate.shape[0]
    expert_count = experts_here * lax.axis_size("sp")
    capacity = max(2, 4 * dev_rows // expert_count)
    flat_ids = route_ids.reshape(-1)
    targets = flat_ids * capacity + slot_numbers(flat_ids)
    slot_ids = lax.broadcasted_iota(jnp.int32, (expert_count * capacity, dev_rows, 2), 0)
    placement_matrix = jnp.sum(
        (targets.reshape(1, dev_rows, 2) == slot_ids).astype(jnp.int32), axis=2
    ).astype(jnp.bfloat16)
    outgoing = jnp.dot(placement_matrix, normed, preferred_element_type=jnp.float32).astype(
        jnp.bfloat16
    )
    outgoing = outgoing.reshape(lax.axis_size("sp"), experts_here, capacity, model_width)
    full_gate, full_up, full_down = (
        lax.all_gather(w_gate, "tp", axis=2, tiled=True),
        lax.all_gather(w_up, "tp", axis=2, tiled=True),
        lax.all_gather(w_down, "tp", axis=2, tiled=True),
    )
    hidden_units = expert_hidden(
        lax.all_to_all(outgoing, "sp", split_axis=0, concat_axis=0, tiled=True), full_gate, full_up
    )
    summed = jnp.einsum(
        "secf,edf->secd", hidden_units, full_down, preferred_element_type=jnp.float32
    )
    returned = send_back(summed.astype(jnp.bfloat16))
    flat_back = returned.reshape(expert_count * capacity, model_width)
    picked = (
        jnp.take(flat_back, targets, axis=0).astype(jnp.float32).reshape(dev_rows, 2, model_width)
    )
    layer_out = carried_wide + jnp.sum(route_weight[..., None] * picked, axis=1)
    return layer_out.astype(jnp.bfloat16)


def solution(mesh):
    placed = (
        P("sp", "tp"),
        P("sp", "tp"),
        P("sp", "tp"),
        P("tp"),
        P(),
        P(),
        P(("sp", "tp"), None),
        P(),
        P(("sp", "tp"), None),
        P(("sp", "tp"), None),
        P("sp", None, "tp"),
        P("sp", None, "tp"),
        P("sp", None, "tp"),
    )
    spread = (
        mesh.shape["sp"] == 8 and mesh.shape["tp"] == 4
    )
    return jax.shard_map(
        spread_layer if spread else local, mesh=mesh, in_specs=placed, out_specs=P(("sp", "tp"), None), check_vma=False
    )
```

```python
import functools

import jax
import jax.numpy as jnp
from jax import lax
from jax.experimental import pallas as pl
from jax.experimental.pallas import tpu as pltpu
from jax.sharding import PartitionSpec as P


EPSILON = 1e-06
OUT_SCALE = 0.8
FLOOR_SCORE = -1e30
LOG2_E = 1.4426950408889634


def place():
    sp, tp = lax.axis_index("sp"), lax.axis_index("tp")
    return sp >> 1, sp & 1, tp >> 1, tp & 1


def moved(value, destination):
    layers = lax.axis_size("sp") // 2
    pairs = []
    for z in range(layers):
        for y in range(2):
            for x in range(2):
                for c in range(2):
                    dz, dy, dx, dc = destination(z, y, x, c)
                    pairs.append(((2 * z + y) * 4 + 2 * x + c, (2 * dz + dy) * 4 + 2 * dx + dc))
    return lax.ppermute(value, ("sp", "tp"), pairs)


def sp_moved(value, mask):
    pairs = [(source, source ^ mask) for source in range(lax.axis_size("sp"))]
    return lax.ppermute(value, "sp", pairs)


def x_swapped(value):
    return moved(value, lambda z, y, x, c: (z, y, 1 - x, c))


def c_swapped(value):
    return moved(value, lambda z, y, x, c: (z, y, x, 1 - c))


def local_call(kernel, out_shapes, operands, in_specs=None, scratch=()):
    shapes = [jax.ShapeDtypeStruct(shape, jnp.bfloat16) for shape in out_shapes]
    vmem = pl.BlockSpec(memory_space=pltpu.VMEM)
    return pl.pallas_call(
        kernel,
        in_specs=in_specs or [vmem] * len(operands),
        out_specs=[vmem] * len(shapes),
        out_shape=shapes,
        scratch_shapes=list(scratch),
    )(*operands)


def pack_kernel(*refs, own_rows, width):
    sources, outs = refs[:3], refs[3:]
    z, _, _, _ = place()
    for k, out in enumerate(outs):
        head, core = (z ^ k) >> 1, (z ^ k) & 1
        for a, source in enumerate(sources):
            for far in range(2):
                start = pl.multiple_of((2 * far + core) * own_rows, own_rows)
                rows = source[pl.ds(start, own_rows), :]
                out[a, far * own_rows : (far + 1) * own_rows, :] = jnp.where(
                    head == 0, rows[:, :width], rows[:, width:]
                )


def pair_kernel(first_ref, second_ref, out_ref):
    keys = first_ref.shape[1]
    out_ref[:, :keys, :] = first_ref[1:]
    out_ref[:, keys:, :] = second_ref[1:]


def attention_kernel(lam_ref, other_lam_ref, *refs, messages, held, far, head_dim):
    message_refs, held_refs = refs[:messages], refs[messages : messages + held]
    gain_ref, out_ref = refs[messages + held], refs[messages + held + 1]
    z, _, x, c = place()
    own_rows = message_refs[0].shape[1] // 2
    start = pl.multiple_of((x ^ far) * own_rows, own_rows)
    query = jnp.concatenate([ref[0, pl.ds(start, own_rows), :] for ref in message_refs], axis=0)
    lam = jnp.where((z >> 1) == c, lam_ref[z & 1], other_lam_ref[z & 1])
    rows = query.shape[0]
    value_dim = 2 * head_dim
    first_map = lax.broadcasted_iota(jnp.int32, query.shape, 1) < head_dim
    zeros = jnp.zeros_like(query)
    both = jnp.concatenate(
        [jnp.where(first_map, query, zeros), jnp.where(first_map, zeros, query)], axis=0
    )
    factor = head_dim ** (-0.5) * LOG2_E
    peak = jnp.full((2 * rows, 1), FLOOR_SCORE, jnp.float32)
    total = jnp.zeros((2 * rows, 2 * value_dim), jnp.float32)
    for piece in held_refs:
        scores = lax.dot_general(
            both, piece[0], (((1,), (1,)), ((), ())), preferred_element_type=jnp.float32
        )
        new_peak = jnp.maximum(peak, jnp.max(scores, axis=1, keepdims=True))
        weights = jnp.exp2((scores - new_peak) * factor).astype(jnp.bfloat16)
        shrink = jnp.exp2((peak - new_peak) * factor)
        value = piece[1]
        extended = jnp.concatenate([value, jnp.ones_like(value)], axis=1)
        total = total * shrink + jnp.dot(weights, extended, preferred_element_type=jnp.float32)
        peak = new_peak
    heads_out = total[:, :value_dim] / total[:, value_dim:]
    combined = heads_out[:rows] - lam * heads_out[rows:]
    mean_square = jnp.mean(combined * combined, axis=1, keepdims=True)
    normalized = combined * lax.rsqrt(mean_square + EPSILON) * gain_ref[...] * OUT_SCALE
    out_ref[...] = normalized.astype(jnp.bfloat16)


def attention(far, lambdas, other_lambdas, messages, held, gain):
    width = messages[0].shape[2]
    rows = len(messages) * messages[0].shape[1] // 2
    smem, vmem = pl.BlockSpec(memory_space=pltpu.SMEM), pl.BlockSpec(memory_space=pltpu.VMEM)
    kernel = functools.partial(
        attention_kernel, messages=len(messages), held=len(held), far=far, head_dim=width // 2
    )
    operands = (lambdas, other_lambdas, *messages, *held, gain.reshape(1, width))
    specs = [smem, smem] + [vmem] * (len(operands) - 2)
    return local_call(kernel, [(rows, width)], operands, specs)[0]


def chosen(ids_ref, owner, rows):
    own_rows = ids_ref.shape[1]
    numbers = lax.broadcasted_iota(jnp.int32, (rows, own_rows), 0)
    first, second = ids_ref[2 * owner : 2 * owner + 1, :], ids_ref[2 * owner + 1 : 2 * owner + 2, :]
    return ((numbers == first) | (numbers == second)).astype(jnp.float32).astype(jnp.bfloat16)


def gather_kernel(ids_ref, own_ref, came_ref, *outs, layers, capacity):
    z, _, x, c = place()
    devices = 2 * layers
    own_rows = ids_ref.shape[1]
    for owner in range(layers):
        start = pl.multiple_of((((z & 1) * 2 + c) ^ z ^ owner) * own_rows, own_rows)
        own, came = own_ref[pl.ds(start, own_rows), :], came_ref[pl.ds(start, own_rows), :]
        heads = jnp.concatenate(
            [jnp.where(x == 0, own, came), jnp.where(x == 0, came, own)], axis=1
        )
        picked = jnp.dot(
            chosen(ids_ref, owner, devices * capacity), heads, preferred_element_type=jnp.float32
        ).astype(jnp.bfloat16)
        for q in range(devices):
            outs[q][owner ^ (q >> 1)] = picked[q * capacity : (q + 1) * capacity]


def relay_kernel(ids_ref, rows_ref, *outs, owner, capacity):
    rows = jnp.dot(
        chosen(ids_ref, owner, len(outs) * capacity),
        rows_ref[...],
        preferred_element_type=jnp.float32,
    ).astype(jnp.bfloat16)
    for m, out in enumerate(outs):
        out[...] = rows[m * capacity : (m + 1) * capacity]


def expert_kernel(*refs, layers, side):
    devices = 2 * layers
    shards = 4
    parts, residuals = refs[:devices], refs[devices : devices + layers]
    gain_ref, w_ref = refs[devices + layers : devices + layers + 2]
    used = devices + layers + 2
    weight_refs = refs[used : used + 3 * shards]
    used += 3 * shards
    outs = refs[used : used + layers]
    w_vmem, gate_vmem, up_vmem, down_vmem, w_sems, sems = refs[used + layers :]
    z, _, _, _ = place()
    value_dim = parts[0].shape[2] // 2
    hidden_dim = weight_refs[0].shape[1]
    w_copies = []
    for h in range(layers):
        for far in range(2):
            start = pl.multiple_of((layers * far + (z ^ h)) * value_dim, value_dim)
            w_copies.append(
                pltpu.make_async_copy(
                    w_ref.at[pl.ds(start, value_dim), :],
                    w_vmem.at[pl.ds((2 * h + far) * value_dim, value_dim), :],
                    w_sems.at[2 * h + far],
                )
            )
    copies = {}
    for s in range(shards):
        columns = pl.ds(s * hidden_dim, hidden_dim)
        for kind, buffer in enumerate((gate_vmem, up_vmem, down_vmem)):
            copies[kind, s] = pltpu.make_async_copy(
                weight_refs[3 * s + kind], buffer.at[:, columns], sems.at[kind, s]
            )
    for copy in w_copies:
        copy.start()
    for copy in copies.values():
        copy.start()
    blocks = [(u, b) for u in range(layers // 2) for b in range(2)]
    attended = jnp.concatenate(
        [
            jnp.concatenate(
                [parts[2 * h + b][side * (layers // 2) + u] for h in range(layers)], axis=1
            )
            for u, b in blocks
        ],
        axis=0,
    )
    residual = jnp.concatenate([residuals[2 * u + b][...] for u, b in blocks], axis=0)
    for copy in w_copies:
        copy.wait()
    mixed = jnp.dot(attended, w_vmem[...], preferred_element_type=jnp.float32)
    carried = (
        residual.astype(jnp.float32) + mixed.astype(jnp.bfloat16).astype(jnp.float32)
    ).astype(jnp.bfloat16)
    rows = normalize(carried.astype(jnp.float32), gain_ref[...])
    hidden = []
    for s in range(shards):
        columns = slice(s * hidden_dim, (s + 1) * hidden_dim)
        copies[0, s].wait()
        gate = jnp.dot(rows, gate_vmem[:, columns], preferred_element_type=jnp.float32)
        copies[1, s].wait()
        up = jnp.dot(rows, up_vmem[:, columns], preferred_element_type=jnp.float32)
        hidden.append((gate / (1.0 + jnp.exp(-gate)) * up).astype(jnp.bfloat16))
    hidden = jnp.concatenate(hidden, axis=1)
    for s in range(shards):
        copies[2, s].wait()
    total = lax.dot_general(
        hidden, down_vmem[...], (((1,), (1,)), ((), ())), preferred_element_type=jnp.float32
    )
    capacity = outs[0].shape[0]
    for n, out in enumerate(outs):
        out[...] = total[n * capacity : (n + 1) * capacity].astype(jnp.bfloat16)


def expert(side, parts, residuals, w_out, norm_gain, shards):
    layers = len(residuals)
    weights = [weight for shard in shards for weight in shard]
    model_width, hidden = w_out.shape[1], weights[0].shape[1]
    capacity = parts[0].shape[1]
    anywhere, vmem = pl.BlockSpec(memory_space=pl.ANY), pl.BlockSpec(memory_space=pltpu.VMEM)
    buffer = pltpu.VMEM((model_width, len(shards) * hidden), jnp.bfloat16)
    return local_call(
        functools.partial(expert_kernel, layers=layers, side=side),
        [(capacity, model_width)] * layers,
        (*parts, *residuals, norm_gain.reshape(1, model_width), w_out, *weights),
        [vmem] * (len(parts) + layers + 1) + [anywhere] * (1 + len(weights)),
        [
            pltpu.VMEM(w_out.shape, jnp.bfloat16),
            buffer,
            buffer,
            buffer,
            pltpu.SemaphoreType.DMA((len(parts),)),
            pltpu.SemaphoreType.DMA((3, len(shards))),
        ],
    )


def combine_kernel(ids_ref, weight_ref, carried_ref, *refs):
    results, out_ref = refs[:-1], refs[-1]
    own_rows = carried_ref.shape[0]
    capacity = results[0].shape[0]
    columns = lax.broadcasted_iota(jnp.int32, (own_rows, len(results) * capacity), 1)
    everything = jnp.concatenate([ref[...] for ref in results], axis=0)
    total = carried_ref[...].astype(jnp.float32)
    summed = None
    for k in range(2):
        pick = (columns == ids_ref[:, k : k + 1]).astype(jnp.float32).astype(jnp.bfloat16)
        part = jnp.dot(pick, everything, preferred_element_type=jnp.float32)
        part = weight_ref[:, k : k + 1] * part
        summed = part if summed is None else summed + part
    out_ref[...] = (total + summed).astype(jnp.bfloat16)


def slot_numbers(flat_ids):
    count_ids = flat_ids.shape[0]
    positions = lax.broadcasted_iota(jnp.int32, (count_ids, count_ids), 0)
    earlier = lax.broadcasted_iota(jnp.int32, (count_ids, count_ids), 1) < positions
    matches = (flat_ids[:, None] == flat_ids[None, :]) & earlier
    return jnp.sum(matches.astype(jnp.int32), axis=1)


def normalize(carried_wide, norm_gain):
    return (
        carried_wide
        * lax.rsqrt(jnp.mean(carried_wide * carried_wide, axis=-1, keepdims=True) + EPSILON)
        * norm_gain
    ).astype(jnp.bfloat16)


def spread_layer(
    queries, keys, values, lambdas, head_gain, w_out, residual_in, norm_gain,
    route_ids, route_weight, w_gate, w_up, w_down,
):
    devices = lax.axis_size("sp")
    layers = devices // 2
    width = queries.shape[1] // 2
    own_rows, model_width = residual_in.shape
    expert_count = w_gate.shape[0] * devices
    capacity = max(2, 4 * own_rows // expert_count)
    z, _, x, c = place()

    gate, up, down = w_gate[0], w_up[0], w_down[0]
    gate_far = x_swapped(gate)
    up_far = x_swapped(up)
    down_far = x_swapped(down)
    shards = [
        [gate, up, down],
        [c_swapped(gate), c_swapped(up), c_swapped(down)],
        [gate_far, up_far, down_far],
        [c_swapped(gate_far), c_swapped(up_far), c_swapped(down_far)],
    ]

    packed = local_call(
        functools.partial(pack_kernel, own_rows=own_rows, width=width),
        [(3, 2 * own_rows, width)] * layers,
        (queries, keys, values),
    )
    messages = [
        moved(packed[k], lambda z, y, x, c: (2 * c + ((z ^ k) >> 1), y, x, (z ^ k) & 1))
        for k in range(layers)
    ]
    other_lambdas = c_swapped(lambdas)
    pairs = [
        local_call(pair_kernel, [(2, 4 * own_rows, width)], (messages[k], messages[k + 1]))[0]
        for k in range(0, layers, 2)
    ]
    chip = pairs + [moved(pair, lambda z, y, x, c: (z, 1 - y, x, c)) for pair in pairs]
    held = chip + [c_swapped(piece) for piece in chip]

    flat_ids = route_ids.reshape(-1)
    targets = (flat_ids * capacity + slot_numbers(flat_ids)).reshape(own_rows, 2).T
    owners = [targets] + [sp_moved(targets, 2 * w) for w in range(1, layers)]
    owners = jnp.concatenate(owners, axis=0)
    ids = ((owners // capacity) ^ lax.axis_index("sp")) * capacity + owners % capacity

    partner = sp_moved(residual_in, devices // 2)
    residuals = []
    for owner, held_rows in ((layers // 2, partner), (0, residual_in)):
        relayed = local_call(
            functools.partial(relay_kernel, owner=owner, capacity=capacity),
            [(capacity, model_width)] * layers,
            (ids, held_rows),
        )
        residuals.append([relayed[0]] + [sp_moved(relayed[m], m) for m in range(1, layers)])

    other_att = attention(1, lambdas, other_lambdas, messages, held, head_gain)
    came_att = x_swapped(other_att)
    own_att = attention(0, lambdas, other_lambdas, messages, held, head_gain)

    gathered = local_call(
        functools.partial(gather_kernel, layers=layers, capacity=capacity),
        [(layers, capacity, 2 * width)] * devices,
        (ids, own_att, came_att),
    )
    parts = [gathered[0]] + [sp_moved(gathered[q], q) for q in range(1, devices)]
    back = {}
    for chunk in range(2):
        results = expert(1 - chunk, parts, residuals[chunk], w_out, norm_gain, shards)
        for i, result in enumerate(results):
            n = (1 - chunk) * layers + i
            back[n] = sp_moved(result, n) if n else result

    pair = jnp.stack(
        [own_att.reshape(layers, own_rows, width), came_att.reshape(layers, own_rows, width)],
        axis=1,
    )
    source = (z & 1) * 2 + c
    collected = []
    for step in range(layers):
        part = lax.dynamic_index_in_dim(pair, source ^ z ^ step, 0, keepdims=False)
        collected.append(sp_moved(part, 2 * step) if step else part)
    everything = jnp.stack(collected)
    ordered = []
    for head_x in range(2):
        for head_z in range(layers):
            row = lax.dynamic_index_in_dim(everything, z ^ head_z, 0, keepdims=False)
            ordered.append(lax.dynamic_index_in_dim(row, x ^ head_x, 0, keepdims=False))
    attended = jnp.concatenate(ordered, axis=1)
    mixed_out = jnp.dot(attended, w_out, preferred_element_type=jnp.float32).astype(jnp.bfloat16)
    carried = (residual_in.astype(jnp.float32) + mixed_out.astype(jnp.float32)).astype(jnp.bfloat16)
    return local_call(
        combine_kernel,
        [(own_rows, model_width)],
        (ids[:2].T, route_weight, carried, *[back[n] for n in range(devices)]),
    )[0]


def swapped(value, axis, distance):
    mask = 2**distance
    pairs = [(source, source ^ mask) for source in range(lax.axis_size(axis))]
    return lax.ppermute(value, axis, pairs)


def block_length(total_rows):
    largest = 1
    for divisor in range(1, min(total_rows, 1024) + 1):
        if total_rows % divisor == 0:
            largest = divisor
    return largest


def expert_hidden(arrived, gate_weight, up_weight):
    gate_proj = jnp.einsum(
        "secd,edf->secf", arrived, gate_weight, preferred_element_type=jnp.float32
    )
    up_proj = jnp.einsum("secd,edf->secf", arrived, up_weight, preferred_element_type=jnp.float32)
    return (jax.nn.silu(gate_proj) * up_proj).astype(jnp.bfloat16)


def send_back(results):
    return lax.all_to_all(results, "sp", split_axis=0, concat_axis=0, tiled=True)


def local(
    queries,
    keys,
    values,
    lambdas,
    head_gain,
    w_out,
    residual_in,
    norm_gain,
    route_ids,
    route_weight,
    w_gate,
    w_up,
    w_down,
):
    tok_rows = queries.shape[0]
    local_heads = lambdas.shape[0]
    head_dim = queries.shape[1] // (2 * local_heads)
    value_dim = 2 * head_dim
    score_scale = head_dim ** (-0.5)
    query_view = queries.reshape(tok_rows, local_heads, 2, head_dim)

    def absorb(running, key_piece, value_piece):
        key_count = key_piece.shape[0]
        step_rows = block_length(key_count)
        key_blocks = key_piece.reshape(key_count // step_rows, step_rows, local_heads, 2, head_dim)
        value_blocks = value_piece.reshape(
            key_count // step_rows, step_rows, local_heads, value_dim
        )

        def one_block(state, block_pair):
            key_block, value_block = block_pair
            running_max, running_sum, running_acc = state
            scores = (
                jnp.einsum(
                    "qhmd,khmd->hmqk", query_view, key_block, preferred_element_type=jnp.float32
                )
                * score_scale
            )
            new_max = jnp.maximum(running_max, jnp.max(scores, axis=-1))
            weights = jnp.exp(scores - new_max[..., None])
            shrink = jnp.exp(running_max - new_max)
            new_sum = running_sum * shrink + jnp.sum(weights, axis=-1)
            product = jnp.einsum(
                "hmqk,khv->hmqv",
                weights.astype(jnp.bfloat16),
                value_block,
                preferred_element_type=jnp.float32,
            )
            return ((new_max, new_sum, running_acc * shrink[..., None] + product), None)

        final_state, _ = lax.scan(one_block, running, (key_blocks, value_blocks))
        return final_state

    initial = (
        jnp.full((local_heads, 2, tok_rows), FLOOR_SCORE, jnp.float32),
        jnp.zeros((local_heads, 2, tok_rows), jnp.float32),
        jnp.zeros((local_heads, 2, tok_rows, value_dim), jnp.float32),
    )
    seq_bits = min(4, lax.axis_size("sp").bit_length() - 1)
    held_keys, held_values = (keys, values)
    state = absorb(initial, held_keys, held_values)
    for bit_number in range(seq_bits):
        came_keys, came_values = swapped((held_keys, held_values), "sp", bit_number)
        state = absorb(state, came_keys, came_values)
        if bit_number + 1 < seq_bits:
            held_keys = jnp.concatenate([held_keys, came_keys], axis=0)
            held_values = jnp.concatenate([held_values, came_values], axis=0)
    _, totals, numerators = state
    heads_out = numerators / totals[..., None]
    combined = heads_out[:, 0] - lambdas[:, None, None] * heads_out[:, 1]
    mean_square = jnp.mean(combined * combined, axis=-1, keepdims=True)
    normalized = combined * lax.rsqrt(mean_square + EPSILON) * head_gain * OUT_SCALE
    attended = (
        jnp.transpose(normalized, (1, 0, 2))
        .reshape(tok_rows, local_heads * value_dim)
        .astype(jnp.bfloat16)
    )
    dev_rows = residual_in.shape[0]
    head_width = attended.shape[1]
    own_rows = lax.dynamic_slice_in_dim(w_out, lax.axis_index("tp") * head_width, head_width, 0)
    mixed_sum = lax.psum_scatter(
        jnp.dot(attended, own_rows, preferred_element_type=jnp.float32).astype(jnp.bfloat16),
        "tp",
        scatter_dimension=0,
        tiled=True,
    )
    carried = (residual_in.astype(jnp.float32) + mixed_sum.astype(jnp.float32)).astype(jnp.bfloat16)
    carried_wide = carried.astype(jnp.float32)
    normed = (
        carried_wide
        * lax.rsqrt(jnp.mean(carried_wide * carried_wide, axis=-1, keepdims=True) + EPSILON)
        * norm_gain
    ).astype(jnp.bfloat16)
    model_width = normed.shape[1]
    experts_here = w_gate.shape[0]
    expert_count = experts_here * lax.axis_size("sp")
    capacity = max(2, 4 * dev_rows // expert_count)
    flat_ids = route_ids.reshape(-1)
    targets = flat_ids * capacity + slot_numbers(flat_ids)
    slot_ids = lax.broadcasted_iota(jnp.int32, (expert_count * capacity, dev_rows, 2), 0)
    placement_matrix = jnp.sum(
        (targets.reshape(1, dev_rows, 2) == slot_ids).astype(jnp.int32), axis=2
    ).astype(jnp.bfloat16)
    outgoing = jnp.dot(placement_matrix, normed, preferred_element_type=jnp.float32).astype(
        jnp.bfloat16
    )
    outgoing = outgoing.reshape(lax.axis_size("sp"), experts_here, capacity, model_width)
    full_gate, full_up, full_down = (
        lax.all_gather(w_gate, "tp", axis=2, tiled=True),
        lax.all_gather(w_up, "tp", axis=2, tiled=True),
        lax.all_gather(w_down, "tp", axis=2, tiled=True),
    )
    hidden_units = expert_hidden(
        lax.all_to_all(outgoing, "sp", split_axis=0, concat_axis=0, tiled=True), full_gate, full_up
    )
    summed = jnp.einsum(
        "secf,edf->secd", hidden_units, full_down, preferred_element_type=jnp.float32
    )
    returned = send_back(summed.astype(jnp.bfloat16))
    flat_back = returned.reshape(expert_count * capacity, model_width)
    picked = (
        jnp.take(flat_back, targets, axis=0).astype(jnp.float32).reshape(dev_rows, 2, model_width)
    )
    layer_out = carried_wide + jnp.sum(route_weight[..., None] * picked, axis=1)
    return layer_out.astype(jnp.bfloat16)


def solution(mesh):
    placed = (
        P("sp", "tp"),
        P("sp", "tp"),
        P("sp", "tp"),
        P("tp"),
        P(),
        P(),
        P(("sp", "tp"), None),
        P(),
        P(("sp", "tp"), None),
        P(("sp", "tp"), None),
        P("sp", None, "tp"),
        P("sp", None, "tp"),
        P("sp", None, "tp"),
    )
    spread = (
        mesh.shape["sp"] == 8 and mesh.shape["tp"] == 4
    )
    if not spread:
        return jax.shard_map(
            local, mesh=mesh, in_specs=placed, out_specs=P(("sp", "tp"), None), check_vma=False
        )

    return jax.shard_map(
        spread_layer, mesh=mesh, in_specs=placed, out_specs=P(("sp", "tp"), None), check_vma=False
    )
```

```python
import functools

import jax
import jax.numpy as jnp
from jax import lax
from jax.experimental import pallas as pl
from jax.experimental.pallas import tpu as pltpu
from jax.sharding import PartitionSpec as P


EPSILON = 1e-06
OUT_SCALE = 0.8
FLOOR_SCORE = -1e30
LOG2_E = 1.4426950408889634


def place():
    sp, tp = lax.axis_index("sp"), lax.axis_index("tp")
    return sp >> 1, sp & 1, tp >> 1, tp & 1


def moved(value, destination):
    layers = lax.axis_size("sp") // 2
    pairs = []
    for z in range(layers):
        for y in range(2):
            for x in range(2):
                for c in range(2):
                    dz, dy, dx, dc = destination(z, y, x, c)
                    pairs.append(((2 * z + y) * 4 + 2 * x + c, (2 * dz + dy) * 4 + 2 * dx + dc))
    return lax.ppermute(value, ("sp", "tp"), pairs)


def sp_moved(value, mask):
    pairs = [(source, source ^ mask) for source in range(lax.axis_size("sp"))]
    return lax.ppermute(value, "sp", pairs)


def x_swapped(value):
    return moved(value, lambda z, y, x, c: (z, y, 1 - x, c))


def c_swapped(value):
    return moved(value, lambda z, y, x, c: (z, y, x, 1 - c))


def local_call(kernel, out_shapes, operands, in_specs=None, scratch=(), dtype=jnp.bfloat16, limit=24):
    shapes = [jax.ShapeDtypeStruct(shape, dtype) for shape in out_shapes]
    vmem = pl.BlockSpec(memory_space=pltpu.VMEM)
    return pl.pallas_call(
        kernel,
        in_specs=in_specs or [vmem] * len(operands),
        out_specs=[vmem] * len(shapes),
        out_shape=shapes,
        scratch_shapes=list(scratch),
        compiler_params=pltpu.CompilerParams(vmem_limit_bytes=limit << 20),
    )(*operands)


def pack_kernel(*refs, own_rows, width):
    sources, outs = refs[:3], refs[3:]
    z, _, _, _ = place()
    for k, out in enumerate(outs):
        head, core = (z ^ k) >> 1, (z ^ k) & 1
        for a, source in enumerate(sources):
            for far in range(2):
                start = pl.multiple_of((2 * far + core) * own_rows, own_rows)
                rows = source[pl.ds(start, own_rows), :]
                out[a, far * own_rows : (far + 1) * own_rows, :] = jnp.where(
                    head == 0, rows[:, :width], rows[:, width:]
                )


def pair_kernel(first_ref, second_ref, out_ref):
    keys = first_ref.shape[1]
    out_ref[:, :keys, :] = first_ref[1:]
    out_ref[:, keys:, :] = second_ref[1:]


def both_maps(message_refs, far, head_dim):
    _, _, x, _ = place()
    own_rows = message_refs[0].shape[1] // 2
    start = pl.multiple_of((x ^ far) * own_rows, own_rows)
    query = jnp.concatenate([ref[0, pl.ds(start, own_rows), :] for ref in message_refs], axis=0)
    first_map = lax.broadcasted_iota(jnp.int32, query.shape, 1) < head_dim
    zeros = jnp.zeros_like(query)
    return jnp.concatenate(
        [jnp.where(first_map, query, zeros), jnp.where(first_map, zeros, query)], axis=0
    )


def absorb(both, held_refs, peak, total, head_dim):
    factor = head_dim ** (-0.5) * LOG2_E
    for piece in held_refs:
        scores = lax.dot_general(
            both, piece[0], (((1,), (1,)), ((), ())), preferred_element_type=jnp.float32
        )
        new_peak = jnp.maximum(peak, jnp.max(scores, axis=1, keepdims=True))
        weights = jnp.exp2((scores - new_peak) * factor).astype(jnp.bfloat16)
        shrink = jnp.exp2((peak - new_peak) * factor)
        value = piece[1]
        extended = jnp.concatenate([value, jnp.ones_like(value)], axis=1)
        total = total * shrink + jnp.dot(weights, extended, preferred_element_type=jnp.float32)
        peak = new_peak
    return peak, total


def early_kernel(*refs, messages, held, far, head_dim):
    message_refs, held_refs = refs[:messages], refs[messages : messages + held]
    out_ref = refs[messages + held]
    both = both_maps(message_refs, far, head_dim)
    peak = jnp.full((out_ref.shape[0], 1), FLOOR_SCORE, jnp.float32)
    total = jnp.zeros(out_ref.shape, jnp.float32)
    peak, total = absorb(both, held_refs, peak, total, head_dim)
    column = lax.broadcasted_iota(jnp.int32, total.shape, 1)
    out_ref[...] = jnp.where(column < 3 * head_dim, total, peak)


def attention_kernel(
    lam_ref, other_lam_ref, state_ref, *refs, messages, held, far, head_dim
):
    message_refs, held_refs = refs[:messages], refs[messages : messages + held]
    gain_ref, out_ref = refs[messages + held], refs[messages + held + 1]
    z, _, _, c = place()
    lam = jnp.where((z >> 1) == c, lam_ref[z & 1], other_lam_ref[z & 1])
    value_dim = 2 * head_dim
    both = both_maps(message_refs, far, head_dim)
    rows = both.shape[0] // 2
    state = state_ref[...]
    column = lax.broadcasted_iota(jnp.int32, (2 * rows, value_dim), 1)
    carrier = jnp.where(column < head_dim, FLOOR_SCORE, state[:, value_dim:])
    peak = jnp.max(carrier, axis=1, keepdims=True)
    peak, total = absorb(both, held_refs, peak, state, head_dim)
    sums = jnp.max(jnp.where(column < head_dim, total[:, value_dim:], 0.0), axis=1, keepdims=True)
    heads_out = total[:, :value_dim] / sums
    combined = heads_out[:rows] - lam * heads_out[rows:]
    mean_square = jnp.mean(combined * combined, axis=1, keepdims=True)
    normalized = combined * lax.rsqrt(mean_square + EPSILON) * gain_ref[...] * OUT_SCALE
    out_ref[...] = normalized.astype(jnp.bfloat16)


def attention(far, lambdas, other_lambdas, state, messages, held, gain):
    width = messages[0].shape[2]
    smem, vmem = pl.BlockSpec(memory_space=pltpu.SMEM), pl.BlockSpec(memory_space=pltpu.VMEM)
    kernel = functools.partial(
        attention_kernel, messages=len(messages), held=len(held), far=far, head_dim=width // 2
    )
    operands = (lambdas, other_lambdas, state, *messages, *held, gain.reshape(1, width))
    specs = [smem, smem] + [vmem] * (len(operands) - 2)
    return local_call(kernel, [(state.shape[0] // 2, width)], operands, specs)[0]


def relative(numbers, capacity):
    return numbers ^ (lax.axis_index("sp") * capacity)


def chosen(ids_ref, rows, capacity):
    ids = relative(ids_ref[...], capacity)
    numbers = lax.broadcasted_iota(jnp.int32, (rows, ids.shape[1]), 0)
    return ((numbers == ids[0:1, :]) | (numbers == ids[1:2, :])).astype(jnp.float32).astype(
        jnp.bfloat16
    )


def gather_kernel(own_ref, came_ref, *refs, layers, capacity):
    id_refs, outs = refs[:layers], refs[layers:]
    z, _, x, c = place()
    devices = 2 * layers
    own_rows = id_refs[0].shape[1]
    for owner in range(layers):
        start = pl.multiple_of((((z & 1) * 2 + c) ^ z ^ owner) * own_rows, own_rows)
        own, came = own_ref[pl.ds(start, own_rows), :], came_ref[pl.ds(start, own_rows), :]
        heads = jnp.concatenate(
            [jnp.where(x == 0, own, came), jnp.where(x == 0, came, own)], axis=1
        )
        outs[devices + owner][...] = heads
        picked = jnp.dot(
            chosen(id_refs[owner], devices * capacity, capacity), heads, preferred_element_type=jnp.float32
        ).astype(jnp.bfloat16)
        for q in range(devices):
            outs[q][owner ^ (q >> 1)] = picked[q * capacity : (q + 1) * capacity]


def carry_kernel(residual_ref, w_ref, *refs):
    parts, out_ref = refs[:-1], refs[-1]
    attended = jnp.concatenate([part[...] for part in parts], axis=1)
    mixed = jnp.dot(attended, w_ref[...], preferred_element_type=jnp.float32)
    out_ref[...] = (
        residual_ref[...].astype(jnp.float32) + mixed.astype(jnp.bfloat16).astype(jnp.float32)
    ).astype(jnp.bfloat16)


def head_copies(w_ref, w_vmem, sems, layers):
    z, _, _, _ = place()
    value_dim = w_ref.shape[0] // (2 * layers)
    copies = []
    for h in range(layers):
        for far in range(2):
            start = pl.multiple_of((layers * far + (z ^ h)) * value_dim, value_dim)
            copies.append(
                pltpu.make_async_copy(
                    w_ref.at[pl.ds(start, value_dim), :],
                    w_vmem.at[pl.ds((2 * h + far) * value_dim, value_dim), :],
                    sems.at[2 * h + far],
                )
            )
    return copies


def relay_kernel(ids_ref, rows_ref, *outs, capacity):
    rows = jnp.dot(
        chosen(ids_ref, len(outs) * capacity, capacity),
        rows_ref[...],
        preferred_element_type=jnp.float32,
    ).astype(jnp.bfloat16)
    for m, out in enumerate(outs):
        out[...] = rows[m * capacity : (m + 1) * capacity]


def stage_kernel(*refs, layers, shards):
    w_ref, weight_refs = refs[0], refs[1 : 1 + 3 * shards]
    w_vmem, *buffers = refs[1 + 3 * shards : 5 + 3 * shards]
    w_sems, sems = refs[5 + 3 * shards :]
    hidden_dim = weight_refs[0].shape[1]
    copies = head_copies(w_ref, w_vmem, w_sems, layers)
    for s in range(shards):
        columns = pl.ds(s * hidden_dim, hidden_dim)
        for kind, buffer in enumerate(buffers):
            copies.append(
                pltpu.make_async_copy(
                    weight_refs[3 * s + kind], buffer.at[:, columns], sems.at[kind, s]
                )
            )
    for copy in copies:
        copy.start()
    for copy in copies:
        copy.wait()


def staged(w_out, shards, layers):
    weights = [weight for shard in shards for weight in shard]
    shape = (w_out.shape[1], len(shards) * weights[0].shape[1])
    return pl.pallas_call(
        functools.partial(stage_kernel, layers=layers, shards=len(shards)),
        in_specs=[pl.BlockSpec(memory_space=pl.ANY)] * (1 + len(weights)),
        out_specs=[pl.BlockSpec(memory_space=pltpu.VMEM)] * 4,
        out_shape=[pltpu.VMEM(w_out.shape, jnp.bfloat16)]
        + [pltpu.VMEM(shape, jnp.bfloat16)] * 3,
        scratch_shapes=[
            pltpu.SemaphoreType.DMA((2 * layers,)),
            pltpu.SemaphoreType.DMA((3, len(shards))),
        ],
        compiler_params=pltpu.CompilerParams(vmem_limit_bytes=8 << 20),
        name="stage",
    )(w_out, *weights)


def expert_kernel(*refs, layers, side):
    devices = 2 * layers
    parts, residuals = refs[:devices], refs[devices : devices + layers]
    gain_ref, w_ref, gate_ref, up_ref, down_ref = refs[devices + layers : devices + layers + 5]
    outs = refs[devices + layers + 5 :]
    blocks = [(u, b) for u in range(layers // 2) for b in range(2)]
    attended = jnp.concatenate(
        [
            jnp.concatenate(
                [parts[2 * h + b][side * (layers // 2) + u] for h in range(layers)], axis=1
            )
            for u, b in blocks
        ],
        axis=0,
    )
    residual = jnp.concatenate([residuals[2 * u + b][...] for u, b in blocks], axis=0)
    mixed = jnp.dot(attended, w_ref[...], preferred_element_type=jnp.float32)
    carried = (
        residual.astype(jnp.float32) + mixed.astype(jnp.bfloat16).astype(jnp.float32)
    ).astype(jnp.bfloat16)
    rows = normalize(carried.astype(jnp.float32), gain_ref[...])
    gate = jnp.dot(rows, gate_ref[...], preferred_element_type=jnp.float32)
    up = jnp.dot(rows, up_ref[...], preferred_element_type=jnp.float32)
    hidden = (gate / (1.0 + jnp.exp(-gate)) * up).astype(jnp.bfloat16)
    total = lax.dot_general(
        hidden, down_ref[...], (((1,), (1,)), ((), ())), preferred_element_type=jnp.float32
    )
    capacity = outs[0].shape[0]
    columns = outs[0].shape[1]
    for number, out in enumerate(outs):
        n, part = number % layers, number // layers
        out[...] = total[
            n * capacity : (n + 1) * capacity, part * columns : (part + 1) * columns
        ].astype(jnp.bfloat16)


def expert(side, parts, residuals, norm_gain, weights, pieces):
    layers = len(residuals)
    model_width = weights[0].shape[1]
    capacity = parts[0].shape[1]
    return local_call(
        functools.partial(expert_kernel, layers=layers, side=side),
        [(capacity, model_width // pieces)] * (layers * pieces),
        (*parts, *residuals, norm_gain.reshape(1, model_width), *weights),
    )


def weighted_rows(ids, weights, everything):
    columns = lax.broadcasted_iota(jnp.int32, (ids.shape[0], everything.shape[0]), 1)
    summed = None
    for k in range(2):
        pick = (columns == ids[:, k : k + 1]).astype(jnp.float32).astype(jnp.bfloat16)
        part = jnp.dot(pick, everything, preferred_element_type=jnp.float32)
        part = weights[:, k : k + 1] * part
        summed = part if summed is None else summed + part
    return summed


def fold_kernel(ids_ref, weight_ref, *refs, capacity):
    results, out_ref = refs[:-1], refs[-1]
    ids = relative(ids_ref[...], capacity).astype(jnp.float32).T.astype(jnp.int32)
    everything = jnp.concatenate([ref[...] for ref in results], axis=0)
    out_ref[...] = weighted_rows(ids, weight_ref[...].T, everything).astype(jnp.bfloat16)


def combine_kernel(ids_ref, weight_ref, carried_ref, folded_ref, *refs, layers):
    near, far, out_ref = refs[:layers], refs[layers : 2 * layers], refs[-1]
    capacity, columns = far[0].shape
    ids, weights = relative(ids_ref[...], capacity), weight_ref[...]
    direct = [ref[:, :columns] for ref in near] + [ref[...] for ref in far]
    first = weighted_rows(ids, weights, jnp.concatenate(direct, axis=0))
    second = weighted_rows(
        ids, weights, jnp.concatenate([ref[:, columns:] for ref in near], axis=0)
    )
    carried = carried_ref[...].astype(jnp.float32)
    out_ref[:, :columns] = (carried[:, :columns] + first).astype(jnp.bfloat16)
    second = second + folded_ref[...].astype(jnp.float32)
    out_ref[:, columns:] = (carried[:, columns:] + second).astype(jnp.bfloat16)


def slot_numbers(flat_ids):
    count_ids = flat_ids.shape[0]
    positions = lax.broadcasted_iota(jnp.int32, (count_ids, count_ids), 0)
    earlier = lax.broadcasted_iota(jnp.int32, (count_ids, count_ids), 1) < positions
    matches = (flat_ids[:, None] == flat_ids[None, :]) & earlier
    return jnp.sum(matches.astype(jnp.int32), axis=1)


def normalize(carried_wide, norm_gain):
    return (
        carried_wide
        * lax.rsqrt(jnp.mean(carried_wide * carried_wide, axis=-1, keepdims=True) + EPSILON)
        * norm_gain
    ).astype(jnp.bfloat16)


def spread_layer(
    queries, keys, values, lambdas, head_gain, w_out, residual_in, norm_gain,
    route_ids, route_weight, w_gate, w_up, w_down,
):
    devices = lax.axis_size("sp")
    layers = devices // 2
    width = queries.shape[1] // 2
    own_rows, model_width = residual_in.shape
    expert_count = w_gate.shape[0] * devices
    capacity = max(2, 4 * own_rows // expert_count)

    gate, up, down = w_gate[0], w_up[0], w_down[0]
    gate_far = x_swapped(gate)
    up_far = x_swapped(up)
    down_far = x_swapped(down)
    shards = [
        [gate, up, down],
        [c_swapped(gate), c_swapped(up), c_swapped(down)],
        [gate_far, up_far, down_far],
        [c_swapped(gate_far), c_swapped(up_far), c_swapped(down_far)],
    ]

    packed = local_call(
        functools.partial(pack_kernel, own_rows=own_rows, width=width),
        [(3, 2 * own_rows, width)] * layers,
        (queries, keys, values),
    )
    messages = [
        moved(packed[k], lambda z, y, x, c: (2 * c + ((z ^ k) >> 1), y, x, (z ^ k) & 1))
        for k in range(layers)
    ]
    other_lambdas = c_swapped(lambdas)
    pairs = [
        local_call(pair_kernel, [(2, 4 * own_rows, width)], (messages[k], messages[k + 1]))[0]
        for k in range(0, layers, 2)
    ]
    chip = pairs + [moved(pair, lambda z, y, x, c: (z, 1 - y, x, c)) for pair in pairs]
    swapped = [c_swapped(piece) for piece in chip]
    own_keys = [chip[1], chip[0], swapped[1], swapped[0]]
    late_keys = [chip[3], chip[2], swapped[3], swapped[2]]
    states = [
        local_call(
            functools.partial(
                early_kernel, messages=layers, held=len(own_keys), far=far, head_dim=width // 2
            ),
            [(2 * layers * own_rows, 2 * width)],
            (*messages, *own_keys),
            dtype=jnp.float32,
        )[0]
        for far in (0, 1)
    ]

    flat_ids = route_ids.reshape(-1)
    numbered = (flat_ids * capacity + slot_numbers(flat_ids)).reshape(own_rows, 2)
    targets = jnp.tile(numbered.T, (4, 1))
    owners = [targets] + [sp_moved(targets, 2 * w) for w in range(1, layers)]
    partner_weight = sp_moved(jnp.tile(route_weight.T, (4, 1)), layers)

    partner = sp_moved(residual_in, devices // 2)
    residuals = []
    for numbers, held_rows in ((owners[layers // 2], partner), (targets, residual_in)):
        relayed = local_call(
            functools.partial(relay_kernel, capacity=capacity),
            [(capacity, model_width)] * layers,
            (numbers, held_rows),
        )
        residuals.append([relayed[0]] + [sp_moved(relayed[m], m) for m in range(1, layers)])

    other_att = attention(1, lambdas, other_lambdas, states[1], messages, late_keys, head_gain)
    came_att = x_swapped(other_att)
    own_att = attention(0, lambdas, other_lambdas, states[0], messages, late_keys, head_gain)

    gathered = local_call(
        functools.partial(gather_kernel, layers=layers, capacity=capacity),
        [(layers, capacity, 2 * width)] * devices + [(own_rows, 2 * width)] * layers,
        (own_att, came_att, *owners),
    )
    parts = [gathered[0]] + [sp_moved(gathered[q], q) for q in range(1, devices)]
    weights = staged(w_out, shards, layers)
    far_results = expert(1, parts, residuals[0], norm_gain, weights, 2)
    near_results = expert(0, parts, residuals[1], norm_gain, weights, 1)
    fold = [far_results[layers]] + [sp_moved(far_results[layers + m], m) for m in range(1, layers)]
    far = [sp_moved(far_results[m], layers + m) for m in range(layers)]
    near = [near_results[0]] + [sp_moved(near_results[m], m) for m in range(1, layers)]
    folded = local_call(
        functools.partial(fold_kernel, capacity=capacity),
        [(own_rows, model_width // 2)],
        (owners[layers // 2], partner_weight, *fold),
    )[0]
    came_folded = sp_moved(folded, layers)

    own_parts = [gathered[devices]] + [
        sp_moved(gathered[devices + step], 2 * step) for step in range(1, layers)
    ]
    carried = local_call(
        carry_kernel, [(own_rows, model_width)], (residual_in, weights[0], *own_parts)
    )[0]
    return local_call(
        functools.partial(combine_kernel, layers=layers),
        [(own_rows, model_width)],
        (numbered, route_weight, carried, came_folded, *near, *far),
    )[0]


def swapped(value, axis, distance):
    mask = 2**distance
    pairs = [(source, source ^ mask) for source in range(lax.axis_size(axis))]
    return lax.ppermute(value, axis, pairs)


def block_length(total_rows):
    largest = 1
    for divisor in range(1, min(total_rows, 1024) + 1):
        if total_rows % divisor == 0:
            largest = divisor
    return largest


def expert_hidden(arrived, gate_weight, up_weight):
    gate_proj = jnp.einsum(
        "secd,edf->secf", arrived, gate_weight, preferred_element_type=jnp.float32
    )
    up_proj = jnp.einsum("secd,edf->secf", arrived, up_weight, preferred_element_type=jnp.float32)
    return (jax.nn.silu(gate_proj) * up_proj).astype(jnp.bfloat16)


def send_back(results):
    return lax.all_to_all(results, "sp", split_axis=0, concat_axis=0, tiled=True)


def local(
    queries,
    keys,
    values,
    lambdas,
    head_gain,
    w_out,
    residual_in,
    norm_gain,
    route_ids,
    route_weight,
    w_gate,
    w_up,
    w_down,
):
    tok_rows = queries.shape[0]
    local_heads = lambdas.shape[0]
    head_dim = queries.shape[1] // (2 * local_heads)
    value_dim = 2 * head_dim
    score_scale = head_dim ** (-0.5)
    query_view = queries.reshape(tok_rows, local_heads, 2, head_dim)

    def absorb(running, key_piece, value_piece):
        key_count = key_piece.shape[0]
        step_rows = block_length(key_count)
        key_blocks = key_piece.reshape(key_count // step_rows, step_rows, local_heads, 2, head_dim)
        value_blocks = value_piece.reshape(
            key_count // step_rows, step_rows, local_heads, value_dim
        )

        def one_block(state, block_pair):
            key_block, value_block = block_pair
            running_max, running_sum, running_acc = state
            scores = (
                jnp.einsum(
                    "qhmd,khmd->hmqk", query_view, key_block, preferred_element_type=jnp.float32
                )
                * score_scale
            )
            new_max = jnp.maximum(running_max, jnp.max(scores, axis=-1))
            weights = jnp.exp(scores - new_max[..., None])
            shrink = jnp.exp(running_max - new_max)
            new_sum = running_sum * shrink + jnp.sum(weights, axis=-1)
            product = jnp.einsum(
                "hmqk,khv->hmqv",
                weights.astype(jnp.bfloat16),
                value_block,
                preferred_element_type=jnp.float32,
            )
            return ((new_max, new_sum, running_acc * shrink[..., None] + product), None)

        final_state, _ = lax.scan(one_block, running, (key_blocks, value_blocks))
        return final_state

    initial = (
        jnp.full((local_heads, 2, tok_rows), FLOOR_SCORE, jnp.float32),
        jnp.zeros((local_heads, 2, tok_rows), jnp.float32),
        jnp.zeros((local_heads, 2, tok_rows, value_dim), jnp.float32),
    )
    seq_bits = min(4, lax.axis_size("sp").bit_length() - 1)
    held_keys, held_values = (keys, values)
    state = absorb(initial, held_keys, held_values)
    for bit_number in range(seq_bits):
        came_keys, came_values = swapped((held_keys, held_values), "sp", bit_number)
        state = absorb(state, came_keys, came_values)
        if bit_number + 1 < seq_bits:
            held_keys = jnp.concatenate([held_keys, came_keys], axis=0)
            held_values = jnp.concatenate([held_values, came_values], axis=0)
    _, totals, numerators = state
    heads_out = numerators / totals[..., None]
    combined = heads_out[:, 0] - lambdas[:, None, None] * heads_out[:, 1]
    mean_square = jnp.mean(combined * combined, axis=-1, keepdims=True)
    normalized = combined * lax.rsqrt(mean_square + EPSILON) * head_gain * OUT_SCALE
    attended = (
        jnp.transpose(normalized, (1, 0, 2))
        .reshape(tok_rows, local_heads * value_dim)
        .astype(jnp.bfloat16)
    )
    dev_rows = residual_in.shape[0]
    head_width = attended.shape[1]
    own_rows = lax.dynamic_slice_in_dim(w_out, lax.axis_index("tp") * head_width, head_width, 0)
    mixed_sum = lax.psum_scatter(
        jnp.dot(attended, own_rows, preferred_element_type=jnp.float32).astype(jnp.bfloat16),
        "tp",
        scatter_dimension=0,
        tiled=True,
    )
    carried = (residual_in.astype(jnp.float32) + mixed_sum.astype(jnp.float32)).astype(jnp.bfloat16)
    carried_wide = carried.astype(jnp.float32)
    normed = (
        carried_wide
        * lax.rsqrt(jnp.mean(carried_wide * carried_wide, axis=-1, keepdims=True) + EPSILON)
        * norm_gain
    ).astype(jnp.bfloat16)
    model_width = normed.shape[1]
    experts_here = w_gate.shape[0]
    expert_count = experts_here * lax.axis_size("sp")
    capacity = max(2, 4 * dev_rows // expert_count)
    flat_ids = route_ids.reshape(-1)
    targets = flat_ids * capacity + slot_numbers(flat_ids)
    slot_ids = lax.broadcasted_iota(jnp.int32, (expert_count * capacity, dev_rows, 2), 0)
    placement_matrix = jnp.sum(
        (targets.reshape(1, dev_rows, 2) == slot_ids).astype(jnp.int32), axis=2
    ).astype(jnp.bfloat16)
    outgoing = jnp.dot(placement_matrix, normed, preferred_element_type=jnp.float32).astype(
        jnp.bfloat16
    )
    outgoing = outgoing.reshape(lax.axis_size("sp"), experts_here, capacity, model_width)
    full_gate, full_up, full_down = (
        lax.all_gather(w_gate, "tp", axis=2, tiled=True),
        lax.all_gather(w_up, "tp", axis=2, tiled=True),
        lax.all_gather(w_down, "tp", axis=2, tiled=True),
    )
    hidden_units = expert_hidden(
        lax.all_to_all(outgoing, "sp", split_axis=0, concat_axis=0, tiled=True), full_gate, full_up
    )
    summed = jnp.einsum(
        "secf,edf->secd", hidden_units, full_down, preferred_element_type=jnp.float32
    )
    returned = send_back(summed.astype(jnp.bfloat16))
    flat_back = returned.reshape(expert_count * capacity, model_width)
    picked = (
        jnp.take(flat_back, targets, axis=0).astype(jnp.float32).reshape(dev_rows, 2, model_width)
    )
    layer_out = carried_wide + jnp.sum(route_weight[..., None] * picked, axis=1)
    return layer_out.astype(jnp.bfloat16)


def solution(mesh):
    placed = (
        P("sp", "tp"),
        P("sp", "tp"),
        P("sp", "tp"),
        P("tp"),
        P(),
        P(),
        P(("sp", "tp"), None),
        P(),
        P(("sp", "tp"), None),
        P(("sp", "tp"), None),
        P("sp", None, "tp"),
        P("sp", None, "tp"),
        P("sp", None, "tp"),
    )
    spread = (
        mesh.shape["sp"] == 8 and mesh.shape["tp"] == 4
    )
    if not spread:
        return jax.shard_map(
            local, mesh=mesh, in_specs=placed, out_specs=P(("sp", "tp"), None), check_vma=False
        )

    return jax.shard_map(
        spread_layer, mesh=mesh, in_specs=placed, out_specs=P(("sp", "tp"), None), check_vma=False
    )
```
